32 devices in a mesh: sp: 8 (over z, y), tp: 4 (over x, core).
Axes of the slice: x: 2, y: 2, z: 4, core: 2. Of those that a mesh axis runs over, the one named last changes fastest.
Arguments:
- hidden_states: bfloat16 [2048, 4096], P('sp', 'tp'), may hold values from -6 to 6
- norm_gain: float32 [4096], replicated, may hold values from 0.1 to 1.9
- query_weight: bfloat16 [4096, 2048], P('sp', 'tp'), may hold values from -0.09375 to 0.09375
- key_weight: bfloat16 [4096, 2048], P('sp', 'tp'), may hold values from -0.09375 to 0.09375
- value_weight: bfloat16 [4096, 2048], P('sp', 'tp'), may hold values from -0.09375 to 0.09375
- output_gate_weight: bfloat16 [4096, 2048], P('sp', 'tp'), may hold values from -0.09375 to 0.09375
- unit_input_weight: bfloat16 [4096, 2048], P('sp', 'tp'), may hold values from -0.09375 to 0.09375
- unit_gate_weight: bfloat16 [4096, 2048], P('sp', 'tp'), may hold values from -0.09375 to 0.09375
- decay_forward: float32 [16], P('tp'), may hold values from 0 to 16
- decay_backward: float32 [16], P('tp'), may hold values from 0 to 16
- group_gain: float32 [2048], P('tp'), may hold values from 0.1 to 1.9
- group_bias: float32 [2048], P('tp'), may hold values from -3 to 3
- depth_kernel: float32 [31, 2048], P(None, 'tp'), may hold values from -7 to 7
- depth_bias: float32 [2048], P('tp'), may hold values from -3 to 3
- channel_gain: float32 [2048], P('tp'), may hold values from 0.1 to 1.9
- channel_bias: float32 [2048], P('tp'), may hold values from -3 to 3
- retention_out_weight: bfloat16 [2048, 4096], P('tp', 'sp'), may hold values from -0.09375 to 0.09375
- convolution_out_weight: bfloat16 [2048, 4096], P('tp', 'sp'), may hold values from -0.09375 to 0.09375
Outputs:
- mixed_out: bfloat16 [2048, 4096], P(('sp', 'tp'))
The draws below stay inside these ranges and needn't reach their ends.
All inputs are finite; a program needn't handle non-finite values.
Results may differ from the reference program's by a relative error of at most 0.018.
Values may be sent and summed in bfloat16 or wider, within the bound.
A program may use at most 128 MiB of HBM per device.

```python
import jax
import jax.numpy as jnp
from jax import lax

D = 4096
HEADS = 16
HEAD_DIM = 128
RET_WIDTH = 2048
CONV_WIDTH = 2048
KERNEL = 31
BLOCK = 128
TOKENS = 2048
N_TP = 4


def decay_logits(key, salt):
    key_pick, key_slow, key_fast = jax.random.split(jax.random.fold_in(key, salt), 3)
    keeps_state = jax.random.uniform(key_pick, (HEADS,), jnp.float32) < 0.5
    slow_rate = jnp.exp(jax.random.uniform(key_slow, (HEADS,), jnp.float32, jnp.log(0.2), jnp.log(2.0))) / TOKENS
    fast_rate = jnp.exp(jax.random.uniform(key_fast, (HEADS,), jnp.float32, jnp.log(1.0 / 100.0), jnp.log(1.0 / 30.0)))
    decay_rate = jnp.where(keeps_state, slow_rate, fast_rate)
    return -decay_rate - jnp.log(-jnp.expm1(-decay_rate))


def draw_decay_forward(key, part):
    return decay_logits(key, 11)


def draw_decay_backward(key, part):
    return decay_logits(key, 23)


def draw_depth_kernel(key, part):
    key_tap, key_spread = jax.random.split(jax.random.fold_in(key, 5))
    channel = jnp.arange(CONV_WIDTH, dtype=jnp.float32)
    rising = jnp.exp(jnp.log(3.0) * channel / CONV_WIDTH)
    spread = jnp.exp(jax.random.uniform(key_spread, (CONV_WIDTH,), jnp.float32, 0.0, jnp.log(4.0)))
    tap_values = jnp.clip(jax.random.normal(key_tap, (KERNEL, CONV_WIDTH), jnp.float32), -3.0, 3.0)
    return tap_values * (rising * spread)[None, :] / jnp.sqrt(jnp.float32(KERNEL))


def levels(own_key, shape, cuts, least, top_value):
    gain = 1.0
    for dim, blocks in cuts:
        heights = jax.random.uniform(jax.random.fold_in(jax.random.fold_in(own_key, 6), dim), (blocks,), jnp.float32, least / len(cuts), top_value / len(cuts))
        gain = gain * jnp.repeat(jnp.exp(heights), shape[dim] // blocks).reshape((-1,) + (1,) * (len(shape) - 1 - dim))
    return gain


def bell_draw(stream_key, extent, scale, most, shards=(), kind=jnp.bfloat16):
    entries = jax.random.normal(stream_key, extent, jnp.float32) * scale
    if len(shards) > 0:
        entries = levels(stream_key, extent, shards, -0.22, 0.18) * entries
    return jnp.clip(entries, min=-most, max=most).astype(kind)


def setup_inputs(seed: int = 0) -> dict:
    key_list = jax.random.split(jax.random.key(seed), 19)
    hidden_states = bell_draw(key_list[0], (TOKENS, D), 1.0, 6.0, ((0, 8), (1, 4)))
    norm_gain = jnp.clip(1.0 + 0.18 * jax.random.normal(key_list[1], (D,), jnp.float32), 0.1, 1.9)
    query_weight = bell_draw(key_list[2], (D, RET_WIDTH), D ** -0.5, 0.09375, ((0, 8), (1, 4)))
    key_weight = bell_draw(key_list[3], (D, RET_WIDTH), D ** -0.5, 0.09375, ((0, 8), (1, 4)))
    value_weight = bell_draw(key_list[4], (D, RET_WIDTH), D ** -0.5, 0.09375, ((0, 8), (1, 4)))
    output_gate_weight = bell_draw(key_list[5], (D, RET_WIDTH), D ** -0.5, 0.09375, ((0, 8), (1, 4)))
    unit_input_weight = bell_draw(key_list[6], (D, CONV_WIDTH), D ** -0.5, 0.09375, ((0, 8), (1, 4)))
    unit_gate_weight = bell_draw(key_list[7], (D, CONV_WIDTH), D ** -0.5, 0.09375, ((0, 8), (1, 4)))
    decay_forward = draw_decay_forward(jax.random.fold_in(key_list[18], 71), 0)
    decay_backward = draw_decay_backward(jax.random.fold_in(key_list[18], 71), 0)
    group_gain = jnp.clip(1.0 + 0.18 * jax.random.normal(key_list[10], (RET_WIDTH,), jnp.float32), 0.1, 1.9)
    group_bias = bell_draw(key_list[11], (RET_WIDTH,), 0.5, 3.0, ((0, 4),), jnp.float32)
    depth_kernel = draw_depth_kernel(jax.random.fold_in(key_list[18], 71), 0)
    depth_bias = bell_draw(key_list[13], (CONV_WIDTH,), 0.5, 3.0, ((0, 4),), jnp.float32)
    channel_gain = jnp.clip(1.0 + 0.18 * jax.random.normal(key_list[14], (CONV_WIDTH,), jnp.float32), 0.1, 1.9)
    channel_bias = bell_draw(key_list[15], (CONV_WIDTH,), 0.5, 3.0, ((0, 4),), jnp.float32)
    retention_out_weight = bell_draw(key_list[16], (RET_WIDTH, D), (RET_WIDTH + CONV_WIDTH) ** -0.5, 0.09375, ((0, 4), (1, 8)))
    convolution_out_weight = bell_draw(key_list[17], (CONV_WIDTH, D), (RET_WIDTH + CONV_WIDTH) ** -0.5, 0.09375, ((0, 4), (1, 8)))
    return dict(hidden_states=hidden_states, norm_gain=norm_gain, query_weight=query_weight, key_weight=key_weight, value_weight=value_weight, output_gate_weight=output_gate_weight, unit_input_weight=unit_input_weight, unit_gate_weight=unit_gate_weight, decay_forward=decay_forward, decay_backward=decay_backward, group_gain=group_gain, group_bias=group_bias, depth_kernel=depth_kernel, depth_bias=depth_bias, channel_gain=channel_gain, channel_bias=channel_bias, retention_out_weight=retention_out_weight, convolution_out_weight=convolution_out_weight)


EPS = 1e-06
THETA = 10000.0

def rotate(rows, positions):
    half_dim = rows.shape[-1] // 2
    inverse = THETA ** (-jnp.arange(half_dim, dtype=jnp.float32) / half_dim)
    angles = positions.astype(jnp.float32)[:, None] * inverse[None, :]
    cosine = jnp.cos(angles)[:, None, :]
    sine = jnp.sin(angles)[:, None, :]
    widened = rows.astype(jnp.float32)
    first_half = widened[..., :half_dim]
    second_half = widened[..., half_dim:]
    turned = jnp.concatenate([first_half * cosine - second_half * sine, second_half * cosine + first_half * sine], axis=-1)
    return turned.astype(jnp.bfloat16)

def to_blocks(rows):
    return rows.reshape(rows.shape[0] // BLOCK, BLOCK, rows.shape[1], rows.shape[2]).transpose(2, 0, 1, 3)

def from_blocks(blocks):
    return blocks.transpose(1, 2, 0, 3).reshape(blocks.shape[1] * blocks.shape[2], blocks.shape[0], blocks.shape[3])

def blockwise(queries, key_rows, values, log_decay, include_diag):
    block_len = queries.shape[2]
    position = jnp.arange(block_len, dtype=jnp.float32)
    distance = position[:, None] - position[None, :]
    allowed = distance >= 0 if include_diag else distance > 0
    inside = jnp.where(allowed[None], jnp.exp(log_decay[:, None, None] * jnp.maximum(distance, 0.0)[None]), 0.0)
    query_wide = queries.astype(jnp.float32)
    key_wide = key_rows.astype(jnp.float32)
    value_wide = values.astype(jnp.float32)
    scores = jnp.einsum('hnqd,hnkd->hnqk', query_wide, key_wide, precision=lax.Precision.HIGHEST) * inside[:, None]
    inner_part = jnp.einsum('hnqk,hnkd->hnqd', scores, value_wide, precision=lax.Precision.HIGHEST)
    toward_end = jnp.exp(log_decay[:, None] * (block_len - 1.0 - position)[None])
    block_states = jnp.einsum('hnkd,hnke->hnde', key_wide * toward_end[:, None, :, None], value_wide, precision=lax.Precision.HIGHEST)
    block_decay = jnp.exp(log_decay * block_len)[:, None, None]

    def advance(state_now, block_state):
        return (block_decay * state_now + block_state, state_now)
    initial = jnp.zeros((block_states.shape[0], block_states.shape[2], block_states.shape[3]), jnp.float32)
    final_state, earlier = lax.scan(advance, initial, jnp.moveaxis(block_states, 1, 0))
    earlier = jnp.moveaxis(earlier, 0, 1)
    from_start = jnp.exp(log_decay[:, None] * (position + 1.0)[None])
    cross_part = jnp.einsum('hnqd,hnde->hnqe', query_wide * from_start[:, None, :, None], earlier, precision=lax.Precision.HIGHEST)
    return (inner_part + cross_part, final_state)

def group_norm(retained, group_gain, group_bias, gate_rows):
    row_mean = lax.optimization_barrier(jnp.mean(retained, axis=-1, keepdims=True))
    centered = retained - row_mean
    variance = lax.optimization_barrier(jnp.mean(centered * centered, axis=-1, keepdims=True))
    scaled = (centered * lax.rsqrt(variance + EPS)).reshape(retained.shape[0], -1)
    scaled = scaled * group_gain[None, :] + group_bias[None, :]
    return (jax.nn.silu(gate_rows.astype(jnp.float32)) * scaled).astype(jnp.bfloat16)

def reference(hidden_states, norm_gain, query_weight, key_weight, value_weight, output_gate_weight, unit_input_weight, unit_gate_weight, decay_forward, decay_backward, group_gain, group_bias, depth_kernel, depth_bias, channel_gain, channel_bias, retention_out_weight, convolution_out_weight):
    widened = hidden_states.astype(jnp.float32)
    normed = (widened * lax.rsqrt(lax.optimization_barrier(jnp.mean(widened * widened, axis=-1, keepdims=True)) + EPS) * norm_gain[None, :]).astype(jnp.bfloat16)

    def project(weight):
        return jnp.dot(normed, weight, preferred_element_type=jnp.float32).astype(jnp.bfloat16)
    proj_q = project(query_weight)
    proj_k = project(key_weight)
    proj_v = project(value_weight)
    proj_g = project(output_gate_weight)
    proj_a = project(unit_input_weight)
    proj_b = project(unit_gate_weight)
    positions = jnp.arange(TOKENS, dtype=jnp.int32)
    queries = rotate(proj_q.reshape(TOKENS, HEADS, HEAD_DIM), positions)
    key_rows = rotate(proj_k.reshape(TOKENS, HEADS, HEAD_DIM), positions)
    values = proj_v.reshape(TOKENS, HEADS, HEAD_DIM)
    log_forward = jax.nn.log_sigmoid(decay_forward)
    log_backward = jax.nn.log_sigmoid(decay_backward)
    ahead, unused_ahead = blockwise(to_blocks(queries), to_blocks(key_rows), to_blocks(values), log_forward, True)
    behind, unused_behind = blockwise(to_blocks(queries[::-1]), to_blocks(key_rows[::-1]), to_blocks(values[::-1]), log_backward, False)
    retained = from_blocks(ahead) + from_blocks(behind)[::-1]
    retention_rows = group_norm(retained, group_gain, group_bias, proj_g)
    unit = (proj_a.astype(jnp.float32) * jax.nn.sigmoid(proj_b.astype(jnp.float32))).astype(jnp.bfloat16)
    half_kernel = (KERNEL - 1) // 2
    padded = jnp.pad(unit, ((half_kernel, half_kernel), (0, 0)))
    filtered = jnp.broadcast_to(depth_bias[None, :], (TOKENS, CONV_WIDTH))
    for offset in range(KERNEL):
        filtered = filtered + depth_kernel[offset][None, :] * padded[offset:offset + TOKENS].astype(jnp.float32)
    row_mean = lax.optimization_barrier(jnp.sum(filtered, axis=1, keepdims=True)) / CONV_WIDTH
    variance = lax.optimization_barrier(jnp.sum(filtered * filtered, axis=1, keepdims=True)) / CONV_WIDTH - row_mean * row_mean
    leveled = (filtered - row_mean) * lax.rsqrt(variance + EPS) * channel_gain[None, :] + channel_bias[None, :]
    convolution_rows = jax.nn.silu(leveled).astype(jnp.bfloat16)
    ret_group = RET_WIDTH // N_TP
    conv_group = CONV_WIDTH // N_TP
    mixed = jnp.zeros((TOKENS, D), jnp.float32)
    for group in range(N_TP):
        partial_value = jnp.dot(retention_rows[:, group * ret_group:(group + 1) * ret_group], retention_out_weight[group * ret_group:(group + 1) * ret_group], preferred_element_type=jnp.float32)
        partial_value = partial_value + jnp.dot(convolution_rows[:, group * conv_group:(group + 1) * conv_group], convolution_out_weight[group * conv_group:(group + 1) * conv_group], preferred_element_type=jnp.float32)
        rounded = lax.optimization_barrier(partial_value.astype(jnp.bfloat16))
        mixed = mixed + rounded.astype(jnp.float32)
    return mixed.astype(jnp.bfloat16)
```

```python
import jax
import jax.numpy as jnp
from jax import lax
from jax.sharding import PartitionSpec as P

HEAD_DIM = 128
CONV_WIDTH = 2048
KERNEL = 31

EPS = 1e-06
THETA = 10000.0
SIDES = 2
BLOCK = 128


def rotate(rows, cosine, sine):
    half_dim = rows.shape[-1] // 2
    widened = rows.astype(jnp.float32)
    first_half = widened[..., :half_dim]
    second_half = widened[..., half_dim:]
    turned = jnp.concatenate(
        [first_half * cosine - second_half * sine, second_half * cosine + first_half * sine],
        axis=-1,
    )
    return turned.astype(jnp.bfloat16)


def shards(
    hidden_states,
    norm_gain,
    query_weight,
    key_weight,
    value_weight,
    output_gate_weight,
    unit_input_weight,
    unit_gate_weight,
    decay_forward,
    decay_backward,
    group_gain,
    group_bias,
    depth_kernel,
    depth_bias,
    channel_gain,
    channel_bias,
    retention_out_weight,
    convolution_out_weight,
):
    n_sp, n_tp = lax.axis_size("sp"), lax.axis_size("tp")
    n_far = n_sp // SIDES
    place = lax.axis_index("sp")
    side = place % SIDES
    far = place // SIDES
    swap = [(i, i ^ 1) for i in range(n_sp)]
    lines = [[f * SIDES + s for f in range(n_far)] for s in range(SIDES)]

    def across(array):
        return lax.ppermute(array, "sp", swap)

    def mine(pair):
        return jnp.where(side == 0, pair[0], pair[1])

    def theirs(pair):
        return jnp.where(side == 0, pair[1], pair[0])

    rows_here, feats_here = hidden_states.shape
    fine = rows_here // n_tp
    depth = query_weight.shape[0]
    half_rows = n_far * rows_here
    lanes = query_weight.shape[1] // n_far
    heads = lanes // HEAD_DIM

    weights = {
        "a": unit_input_weight,
        "b": unit_gate_weight,
        "k": key_weight,
        "v": value_weight,
        "q": query_weight,
        "g": output_gate_weight,
    }
    other = {name: across(weight) for name, weight in weights.items()}
    ret_other = across(retention_out_weight)
    conv_other = across(convolution_out_weight)

    whole = lax.all_to_all(
        hidden_states.reshape(n_tp, fine, feats_here), "tp", 0, 0, tiled=True
    )
    whole = whole.transpose(1, 0, 2).reshape(fine, n_tp * feats_here)
    widened = whole.astype(jnp.float32)
    normed = (
        widened
        * lax.rsqrt(jnp.mean(widened * widened, axis=-1, keepdims=True) + EPS)
        * norm_gain[None, :]
    ).astype(jnp.bfloat16)
    spread = lax.all_to_all(
        normed.reshape(fine, n_sp, depth).transpose(1, 0, 2), "sp", 0, 0, tiled=True
    )
    halves = spread.reshape(SIDES, n_far, fine, depth)
    joined = jnp.stack([mine(halves), across(theirs(halves))])
    full = lax.all_gather(joined, "tp", axis=0)
    full = full.transpose(1, 2, 0, 3, 4).reshape(2, half_rows, depth)
    x_own, x_other = full[0], full[1]

    def project(names):
        parts = []
        for name in names:
            product = jnp.dot(
                x_own, weights[name], preferred_element_type=jnp.float32
            ) + jnp.dot(x_other, other[name], preferred_element_type=jnp.float32)
            parts.append(product.astype(jnp.bfloat16).reshape(half_rows, n_far, lanes))
        block = jnp.concatenate(parts, axis=2).transpose(1, 0, 2)
        summed = lax.psum_scatter(
            block, "sp", scatter_dimension=0, axis_index_groups=lines, tiled=True
        )[0]
        return [summed[:, i * lanes : (i + 1) * lanes] for i in range(len(names))]

    proj_a, proj_b = project("ab")
    proj_k, proj_v = project("kv")
    proj_q, proj_g = project("qg")

    def own_lanes(array):
        return lax.dynamic_slice_in_dim(array, far * lanes, lanes, axis=array.ndim - 1)

    unit = (proj_a.astype(jnp.float32) * jax.nn.sigmoid(proj_b.astype(jnp.float32))).astype(
        jnp.bfloat16
    )
    reach = (KERNEL - 1) // 2
    got = across(jnp.where(side == 0, unit[half_rows - reach :], unit[:reach]))
    none = jnp.zeros_like(got)
    padded = jnp.concatenate(
        [jnp.where(side == 0, none, got), unit, jnp.where(side == 0, got, none)], axis=0
    ).astype(jnp.float32)
    taps = own_lanes(depth_kernel)
    filtered = jnp.broadcast_to(own_lanes(depth_bias)[None, :], unit.shape)
    for offset in range(KERNEL):
        filtered = filtered + taps[offset][None, :] * padded[offset : offset + half_rows]
    sums = jnp.stack([jnp.sum(filtered, axis=1), jnp.sum(filtered * filtered, axis=1)])
    sums = jnp.stack([jnp.where(side == s, sums, 0.0) for s in range(SIDES)])
    row_sum, row_squares = mine(lax.psum(sums, ("sp", "tp")))
    row_mean = (row_sum / CONV_WIDTH)[:, None]
    variance = (row_squares / CONV_WIDTH)[:, None] - row_mean * row_mean
    leveled = (filtered - row_mean) * lax.rsqrt(variance + EPS) * own_lanes(channel_gain)[
        None, :
    ] + own_lanes(channel_bias)[None, :]
    convolution_rows = jax.nn.silu(leveled).astype(jnp.bfloat16)
    convolution_all = lax.all_gather(
        convolution_rows, "sp", axis=1, axis_index_groups=lines, tiled=True
    )

    local = jnp.arange(half_rows, dtype=jnp.float32)
    half_dim = HEAD_DIM // 2
    inverse = THETA ** (-jnp.arange(half_dim, dtype=jnp.float32) / half_dim)
    positions = (side * half_rows + jnp.arange(half_rows, dtype=jnp.int32)).astype(jnp.float32)
    angles = positions[:, None] * inverse[None, :]
    cosine, sine = jnp.cos(angles), jnp.sin(angles)
    log_forward = jax.nn.log_sigmoid(decay_forward)
    log_backward = jax.nn.log_sigmoid(decay_backward)
    own_gain, own_bias = own_lanes(group_gain), own_lanes(group_bias)
    distance = local[:, None] - local[None, :]
    ready = []
    for h in range(heads):
        span = slice(h * HEAD_DIM, (h + 1) * HEAD_DIM)
        log_f = lax.dynamic_index_in_dim(log_forward, far * heads + h, keepdims=False)
        log_b = lax.dynamic_index_in_dim(log_backward, far * heads + h, keepdims=False)
        keys = rotate(proj_k[:, span], cosine, sine)
        values = proj_v[:, span]
        log_side = jnp.where(side == 0, log_f, log_b)
        to_edge = jnp.where(side == 0, half_rows - 1.0 - local, local)
        state = jnp.dot(
            (keys.astype(jnp.float32) * jnp.exp(log_side * to_edge)[:, None])
            .astype(jnp.bfloat16)
            .T,
            values,
            preferred_element_type=jnp.float32,
        )
        entering = across(state.astype(jnp.bfloat16))
        queries = rotate(proj_q[:, span], cosine, sine)
        decay = jnp.exp(
            jnp.where(distance >= 0, log_f, log_b) * jnp.abs(distance)
        )
        scores = jnp.dot(queries, keys.T, preferred_element_type=jnp.float32) * decay
        inner = jnp.dot(scores.astype(jnp.bfloat16), values, preferred_element_type=jnp.float32)
        log_enter = jnp.where(side == 0, log_b, log_f)
        from_edge = jnp.where(side == 0, half_rows - local, local + 1.0)
        carried = jnp.dot(queries, entering, preferred_element_type=jnp.float32)
        retained = inner + carried * jnp.exp(log_enter * from_edge)[:, None]
        mean = jnp.mean(retained, axis=-1, keepdims=True)
        centered = retained - mean
        spread_out = jnp.mean(centered * centered, axis=-1, keepdims=True)
        scaled = centered * lax.rsqrt(spread_out + EPS)
        scaled = scaled * own_gain[None, span] + own_bias[None, span]
        ready.append(
            (jax.nn.silu(proj_g[:, span].astype(jnp.float32)) * scaled).astype(jnp.bfloat16)
        )
    retention_rows = jnp.concatenate(ready, axis=1) if heads > 1 else ready[0]
    retention_all = lax.all_gather(
        retention_rows, "sp", axis=1, axis_index_groups=lines, tiled=True
    )

    def merge(ret_weight, conv_weight):
        return (
            jnp.dot(retention_all, ret_weight, preferred_element_type=jnp.float32)
            + jnp.dot(convolution_all, conv_weight, preferred_element_type=jnp.float32)
        ).astype(jnp.bfloat16)

    cols = retention_out_weight.shape[1]
    mixed = jnp.stack(
        [
            merge(retention_out_weight, convolution_out_weight),
            merge(ret_other, conv_other),
        ]
    )
    mixed = mixed.reshape(2, n_far, n_tp, fine, cols).transpose(2, 0, 1, 3, 4)
    mixed = lax.psum_scatter(
        mixed.reshape(2 * n_far * n_tp * fine, cols), "tp", scatter_dimension=0, tiled=True
    ).reshape(2, n_far, fine, cols)
    kept, arrived = mixed[0], across(mixed[1])
    home = jnp.where(
        side == 0, jnp.stack([kept, arrived]), jnp.stack([arrived, kept])
    ).reshape(n_sp, fine, cols)
    home = lax.all_to_all(home, "sp", 0, 0, tiled=True)
    return home.transpose(1, 0, 2).reshape(fine, n_sp * cols)


def with_halo(cells, sides, width):
    for axis, dim in sides:
        count = lax.axis_size(axis)
        ends = count - 1
        head = lax.slice_in_dim(cells, 0, width, axis=dim)
        tail = lax.slice_in_dim(cells, cells.shape[dim] - width, cells.shape[dim], axis=dim)
        cells = jnp.concatenate(
            [
                lax.ppermute(tail, axis, [(i, (i + 1) % count) for i in range(ends)]),
                cells,
                lax.ppermute(head, axis, [((i + 1) % count, i) for i in range(ends)]),
            ],
            axis=dim,
        )
    return cells


def rotate_at(rows, positions):
    half_dim = rows.shape[-1] // 2
    inverse = THETA ** (-jnp.arange(half_dim, dtype=jnp.float32) / half_dim)
    angles = positions.astype(jnp.float32)[:, None] * inverse[None, :]
    cosine = jnp.cos(angles)[:, None, :]
    sine = jnp.sin(angles)[:, None, :]
    widened = rows.astype(jnp.float32)
    first_half = widened[..., :half_dim]
    second_half = widened[..., half_dim:]
    turned = jnp.concatenate(
        [first_half * cosine - second_half * sine, second_half * cosine + first_half * sine],
        axis=-1,
    )
    return turned.astype(jnp.bfloat16)


def to_blocks(rows):
    return rows.reshape(rows.shape[0] // BLOCK, BLOCK, rows.shape[1], rows.shape[2]).transpose(
        2, 0, 1, 3
    )


def from_blocks(blocks):
    return blocks.transpose(1, 2, 0, 3).reshape(
        blocks.shape[1] * blocks.shape[2], blocks.shape[0], blocks.shape[3]
    )


def blockwise(queries, key_rows, values, log_decay, include_diag):
    block_len = queries.shape[2]
    position = jnp.arange(block_len, dtype=jnp.float32)
    distance = position[:, None] - position[None, :]
    allowed = distance >= 0 if include_diag else distance > 0
    inside = jnp.where(
        allowed[None], jnp.exp(log_decay[:, None, None] * jnp.maximum(distance, 0.0)[None]), 0.0
    )
    query_wide = queries.astype(jnp.float32)
    key_wide = key_rows.astype(jnp.float32)
    value_wide = values.astype(jnp.float32)
    scores = (
        jnp.einsum("hnqd,hnkd->hnqk", query_wide, key_wide, precision=lax.Precision.HIGHEST)
        * inside[:, None]
    )
    inner_part = jnp.einsum("hnqk,hnkd->hnqd", scores, value_wide, precision=lax.Precision.HIGHEST)
    toward_end = jnp.exp(log_decay[:, None] * (block_len - 1.0 - position)[None])
    block_states = jnp.einsum(
        "hnkd,hnke->hnde",
        key_wide * toward_end[:, None, :, None],
        value_wide,
        precision=lax.Precision.HIGHEST,
    )
    block_decay = jnp.exp(log_decay * block_len)[:, None, None]

    def advance(state_now, block_state):
        return (block_decay * state_now + block_state, state_now)

    initial = jnp.zeros(
        (block_states.shape[0], block_states.shape[2], block_states.shape[3]), jnp.float32
    )
    final_state, earlier = lax.scan(advance, initial, jnp.moveaxis(block_states, 1, 0))
    earlier = jnp.moveaxis(earlier, 0, 1)
    from_start = jnp.exp(log_decay[:, None] * (position + 1.0)[None])
    cross_part = jnp.einsum(
        "hnqd,hnde->hnqe",
        query_wide * from_start[:, None, :, None],
        earlier,
        precision=lax.Precision.HIGHEST,
    )
    return (inner_part + cross_part, final_state)


def group_norm(retained, group_gain, group_bias, gate_rows):
    row_mean = jnp.mean(retained, axis=-1, keepdims=True)
    centered = retained - row_mean
    variance = jnp.mean(centered * centered, axis=-1, keepdims=True)
    scaled = (centered * lax.rsqrt(variance + EPS)).reshape(retained.shape[0], -1)
    scaled = scaled * group_gain[None, :] + group_bias[None, :]
    return (jax.nn.silu(gate_rows.astype(jnp.float32)) * scaled).astype(jnp.bfloat16)


def shards_general(
    hidden_states,
    norm_gain,
    query_weight,
    key_weight,
    value_weight,
    output_gate_weight,
    unit_input_weight,
    unit_gate_weight,
    decay_forward,
    decay_backward,
    group_gain,
    group_bias,
    depth_kernel,
    depth_bias,
    channel_gain,
    channel_bias,
    retention_out_weight,
    convolution_out_weight,
):
    row_total = hidden_states.shape[0]
    whole = lax.all_gather(hidden_states, "tp", axis=1, tiled=True)
    widened = whole.astype(jnp.float32)
    normed = (
        widened
        * lax.rsqrt(jnp.mean(widened * widened, axis=-1, keepdims=True) + EPS)
        * norm_gain[None, :]
    ).astype(jnp.bfloat16)
    slabs = (
        lax.all_gather(query_weight, "sp", axis=0, tiled=True),
        lax.all_gather(key_weight, "sp", axis=0, tiled=True),
        lax.all_gather(value_weight, "sp", axis=0, tiled=True),
        lax.all_gather(output_gate_weight, "sp", axis=0, tiled=True),
        lax.all_gather(unit_input_weight, "sp", axis=0, tiled=True),
        lax.all_gather(unit_gate_weight, "sp", axis=0, tiled=True),
    )
    summed = tuple((jnp.dot(normed, slab, preferred_element_type=jnp.float32) for slab in slabs))
    proj_q, proj_k, proj_v, proj_g, proj_a, proj_b = tuple(
        (part_sum.astype(jnp.bfloat16) for part_sum in summed)
    )
    head_count = proj_q.shape[1] // HEAD_DIM
    device = lax.axis_index("sp")
    positions = device * row_total + jnp.arange(row_total, dtype=jnp.int32)
    queries = rotate_at(proj_q.reshape(row_total, head_count, HEAD_DIM), positions)
    key_rows = rotate_at(proj_k.reshape(row_total, head_count, HEAD_DIM), positions)
    values = proj_v.reshape(row_total, head_count, HEAD_DIM)
    log_forward = jax.nn.log_sigmoid(decay_forward)
    log_backward = jax.nn.log_sigmoid(decay_backward)
    ahead_local, state_ahead = blockwise(
        to_blocks(queries), to_blocks(key_rows), to_blocks(values), log_forward, True
    )
    behind_local, state_behind = blockwise(
        to_blocks(queries[::-1]),
        to_blocks(key_rows[::-1]),
        to_blocks(values[::-1]),
        log_backward,
        False,
    )
    slabs = (
        lax.all_gather(state_ahead[None].astype(jnp.bfloat16), "sp", axis=0, tiled=True).astype(
            jnp.float32
        ),
        lax.all_gather(state_behind[None].astype(jnp.bfloat16), "sp", axis=0, tiled=True).astype(
            jnp.float32
        ),
    )
    source = jnp.arange(slabs[0].shape[0], dtype=jnp.int32)
    gap_ahead = device - 1 - source
    gap_behind = source - device - 1
    weight_ahead = jnp.where(
        gap_ahead[:, None] >= 0,
        jnp.exp(
            log_forward[None, :]
            * row_total
            * jnp.maximum(gap_ahead, 0).astype(jnp.float32)[:, None]
        ),
        0.0,
    )
    weight_behind = jnp.where(
        gap_behind[:, None] >= 0,
        jnp.exp(
            log_backward[None, :]
            * row_total
            * jnp.maximum(gap_behind, 0).astype(jnp.float32)[:, None]
        ),
        0.0,
    )
    enter_ahead = jnp.zeros_like(state_ahead) + jnp.einsum(
        "jh,jhde->hde", weight_ahead, slabs[0], precision=lax.Precision.HIGHEST
    )
    enter_behind = jnp.zeros_like(state_behind) + jnp.einsum(
        "jh,jhde->hde", weight_behind, slabs[1], precision=lax.Precision.HIGHEST
    )
    local_position = jnp.arange(row_total, dtype=jnp.float32)
    lift_ahead = jnp.exp(log_forward[None, :] * (local_position + 1.0)[:, None])
    lift_behind = jnp.exp(log_backward[None, :] * (row_total - local_position)[:, None])
    query_wide = queries.astype(jnp.float32)
    carried = jnp.einsum(
        "shd,hde->she",
        query_wide * lift_ahead[:, :, None],
        enter_ahead,
        precision=lax.Precision.HIGHEST,
    )
    carried = carried + jnp.einsum(
        "shd,hde->she",
        query_wide * lift_behind[:, :, None],
        enter_behind,
        precision=lax.Precision.HIGHEST,
    )
    retained = from_blocks(ahead_local) + from_blocks(behind_local)[::-1] + carried
    retention_rows = group_norm(retained, group_gain, group_bias, proj_g)
    unit = (proj_a.astype(jnp.float32) * jax.nn.sigmoid(proj_b.astype(jnp.float32))).astype(
        jnp.bfloat16
    )
    half_kernel = (KERNEL - 1) // 2
    padded = with_halo(unit, (("sp", 0),), half_kernel)
    filtered = jnp.broadcast_to(depth_bias[None, :], (row_total, unit.shape[1]))
    for offset in range(KERNEL):
        filtered = filtered + depth_kernel[offset][None, :] * padded[
            offset : offset + row_total
        ].astype(jnp.float32)
    row_sum, row_squares = lax.psum(
        (jnp.sum(filtered, axis=1), jnp.sum(filtered * filtered, axis=1)), "tp"
    )
    row_mean = (row_sum / CONV_WIDTH)[:, None]
    variance = (row_squares / CONV_WIDTH)[:, None] - row_mean * row_mean
    leveled = (filtered - row_mean) * lax.rsqrt(variance + EPS) * channel_gain[
        None, :
    ] + channel_bias[None, :]
    convolution_rows = jax.nn.silu(leveled).astype(jnp.bfloat16)
    retention_full, convolution_full = (
        lax.all_gather(retention_out_weight, "sp", axis=1, tiled=True),
        lax.all_gather(convolution_out_weight, "sp", axis=1, tiled=True),
    )
    return lax.psum_scatter(
        (
            jnp.dot(retention_rows, retention_full, preferred_element_type=jnp.float32)
            + jnp.dot(convolution_rows, convolution_full, preferred_element_type=jnp.float32)
        ).astype(jnp.bfloat16),
        "tp",
        scatter_dimension=0,
        tiled=True,
    )


def solution(mesh):
    lines = mesh.shape["sp"] // SIDES
    head_groups = mesh.shape["tp"] * lines
    fits = mesh.shape["sp"] % SIDES == 0 and CONV_WIDTH % (head_groups * HEAD_DIM) == 0
    placed = (
        P("sp", "tp"),
        P(),
        P("sp", "tp"),
        P("sp", "tp"),
        P("sp", "tp"),
        P("sp", "tp"),
        P("sp", "tp"),
        P("sp", "tp"),
        P("tp"),
        P("tp"),
        P("tp"),
        P("tp"),
        P(None, "tp"),
        P("tp"),
        P("tp"),
        P("tp"),
        P("tp", "sp"),
        P("tp", "sp"),
    )
    return jax.shard_map(
        shards if fits else shards_general,
        mesh=mesh, in_specs=placed, out_specs=P(("sp", "tp"), None), check_vma=False
    )
```

```python
import jax
import jax.numpy as jnp
from jax import lax
from jax.sharding import PartitionSpec as P

HEAD_DIM = 128
CONV_WIDTH = 2048
KERNEL = 31

EPS = 1e-06
THETA = 10000.0
SIDES = 2
BLOCK = 128


def rotate(rows, cosine, sine):
    half_dim = rows.shape[-1] // 2
    widened = rows.astype(jnp.float32)
    first_half = widened[..., :half_dim]
    second_half = widened[..., half_dim:]
    turned = jnp.concatenate(
        [first_half * cosine - second_half * sine, second_half * cosine + first_half * sine],
        axis=-1,
    )
    return turned.astype(jnp.bfloat16)


def shards(
    hidden_states,
    norm_gain,
    query_weight,
    key_weight,
    value_weight,
    output_gate_weight,
    unit_input_weight,
    unit_gate_weight,
    decay_forward,
    decay_backward,
    group_gain,
    group_bias,
    depth_kernel,
    depth_bias,
    channel_gain,
    channel_bias,
    retention_out_weight,
    convolution_out_weight,
):
    n_sp, n_tp = lax.axis_size("sp"), lax.axis_size("tp")
    n_far = n_sp // SIDES
    place = lax.axis_index("sp")
    side = place % SIDES
    far = place // SIDES
    swap = [(i, i ^ 1) for i in range(n_sp)]
    lines = [[f * SIDES + s for f in range(n_far)] for s in range(SIDES)]

    def across(array):
        return lax.ppermute(array, "sp", swap)

    def mine(pair):
        return jnp.where(side == 0, pair[0], pair[1])

    def theirs(pair):
        return jnp.where(side == 0, pair[1], pair[0])

    rows_here, feats_here = hidden_states.shape
    fine = rows_here // n_tp
    depth = query_weight.shape[0]
    half_rows = n_far * rows_here
    lanes = query_weight.shape[1] // n_far
    heads = lanes // HEAD_DIM

    weights = {
        "a": unit_input_weight,
        "b": unit_gate_weight,
        "k": key_weight,
        "v": value_weight,
        "q": query_weight,
        "g": output_gate_weight,
    }
    other = {name: across(weight) for name, weight in weights.items()}
    ret_other = across(retention_out_weight)
    conv_other = across(convolution_out_weight)

    whole = lax.all_to_all(
        hidden_states.reshape(n_tp, fine, feats_here), "tp", 0, 0, tiled=True
    )
    whole = whole.transpose(1, 0, 2).reshape(fine, n_tp * feats_here)
    widened = whole.astype(jnp.float32)
    normed = (
        widened
        * lax.rsqrt(jnp.mean(widened * widened, axis=-1, keepdims=True) + EPS)
        * norm_gain[None, :]
    ).astype(jnp.bfloat16)
    spread = lax.all_to_all(
        normed.reshape(fine, n_sp, depth).transpose(1, 0, 2), "sp", 0, 0, tiled=True
    )
    halves = spread.reshape(SIDES, n_far, fine, depth)
    joined = jnp.stack([mine(halves), across(theirs(halves))])
    full = lax.all_gather(joined, "tp", axis=0)
    full = full.transpose(1, 2, 0, 3, 4).reshape(2, half_rows, depth)
    x_own, x_other = full[0], full[1]

    def products(names):
        parts = []
        for name in names:
            product = jnp.dot(
                x_own, weights[name], preferred_element_type=jnp.float32
            ) + jnp.dot(x_other, other[name], preferred_element_type=jnp.float32)
            parts.append(product.astype(jnp.bfloat16).reshape(half_rows, n_far, lanes))
        return jnp.concatenate(parts, axis=2).transpose(1, 0, 2)

    def scatter(block):
        summed = lax.psum_scatter(
            block, "sp", scatter_dimension=0, axis_index_groups=lines, tiled=True
        )[0]
        return [summed[:, i : i + lanes] for i in range(0, summed.shape[1], lanes)]

    def gather_line(rows):
        blocks = [rows]
        for d in range(1, n_far):
            steps = [
                (line[f], line[(f + d) % n_far]) for line in lines for f in range(n_far)
            ]
            blocks.append(lax.ppermute(rows, "sp", steps))
        return jnp.concatenate(blocks, axis=1)

    def line_order(weight):
        return jnp.concatenate(
            [
                lax.dynamic_slice_in_dim(weight, (far - d) % n_far * lanes, lanes, axis=0)
                for d in range(n_far)
            ],
            axis=0,
        )

    proj_a, proj_b = scatter(products("ab"))
    proj_k, proj_v, proj_q = scatter(products("kvq"))
    block_g = products("g")

    def own_lanes(array):
        return lax.dynamic_slice_in_dim(array, far * lanes, lanes, axis=array.ndim - 1)

    unit = (proj_a.astype(jnp.float32) * jax.nn.sigmoid(proj_b.astype(jnp.float32))).astype(
        jnp.bfloat16
    )
    reach = (KERNEL - 1) // 2
    got = across(jnp.where(side == 0, unit[half_rows - reach :], unit[:reach]))
    none = jnp.zeros_like(got)
    padded = jnp.concatenate(
        [jnp.where(side == 0, none, got), unit, jnp.where(side == 0, got, none)], axis=0
    ).astype(jnp.float32)
    taps = own_lanes(depth_kernel)
    filtered = jnp.broadcast_to(own_lanes(depth_bias)[None, :], unit.shape)
    for offset in range(KERNEL):
        filtered = filtered + taps[offset][None, :] * padded[offset : offset + half_rows]
    sums = jnp.stack([jnp.sum(filtered, axis=1), jnp.sum(filtered * filtered, axis=1)])
    row_sum, row_squares = lax.psum(
        lax.psum(sums, "tp"), "sp", axis_index_groups=lines
    )
    row_mean = (row_sum / CONV_WIDTH)[:, None]
    variance = (row_squares / CONV_WIDTH)[:, None] - row_mean * row_mean
    leveled = (filtered - row_mean) * lax.rsqrt(variance + EPS) * own_lanes(channel_gain)[
        None, :
    ] + own_lanes(channel_bias)[None, :]
    convolution_rows = jax.nn.silu(leveled).astype(jnp.bfloat16)
    block_g, convolution_rows = lax.optimization_barrier((block_g, convolution_rows))
    (proj_g,) = scatter(block_g)
    convolution_all = gather_line(convolution_rows)

    local = jnp.arange(half_rows, dtype=jnp.float32)
    half_dim = HEAD_DIM // 2
    inverse = THETA ** (-jnp.arange(half_dim, dtype=jnp.float32) / half_dim)
    positions = (side * half_rows + jnp.arange(half_rows, dtype=jnp.int32)).astype(jnp.float32)
    angles = positions[:, None] * inverse[None, :]
    cosine, sine = jnp.cos(angles), jnp.sin(angles)
    log_forward = jax.nn.log_sigmoid(decay_forward)
    log_backward = jax.nn.log_sigmoid(decay_backward)
    own_gain, own_bias = own_lanes(group_gain), own_lanes(group_bias)
    distance = local[:, None] - local[None, :]
    ready = []
    for h in range(heads):
        span = slice(h * HEAD_DIM, (h + 1) * HEAD_DIM)
        log_f = lax.dynamic_index_in_dim(log_forward, far * heads + h, keepdims=False)
        log_b = lax.dynamic_index_in_dim(log_backward, far * heads + h, keepdims=False)
        keys = rotate(proj_k[:, span], cosine, sine)
        values = proj_v[:, span]
        log_side = jnp.where(side == 0, log_f, log_b)
        to_edge = jnp.where(side == 0, half_rows - 1.0 - local, local)
        state = jnp.dot(
            (keys.astype(jnp.float32) * jnp.exp(log_side * to_edge)[:, None])
            .astype(jnp.bfloat16)
            .T,
            values,
            preferred_element_type=jnp.float32,
        )
        entering = across(state.astype(jnp.bfloat16))
        queries = rotate(proj_q[:, span], cosine, sine)
        decay = jnp.exp(
            jnp.where(distance >= 0, log_f, log_b) * jnp.abs(distance)
        )
        scores = jnp.dot(queries, keys.T, preferred_element_type=jnp.float32) * decay
        inner = jnp.dot(scores.astype(jnp.bfloat16), values, preferred_element_type=jnp.float32)
        log_enter = jnp.where(side == 0, log_b, log_f)
        from_edge = jnp.where(side == 0, half_rows - local, local + 1.0)
        carried = jnp.dot(queries, entering, preferred_element_type=jnp.float32)
        retained = inner + carried * jnp.exp(log_enter * from_edge)[:, None]
        mean = jnp.mean(retained, axis=-1, keepdims=True)
        centered = retained - mean
        spread_out = jnp.mean(centered * centered, axis=-1, keepdims=True)
        scaled = centered * lax.rsqrt(spread_out + EPS)
        scaled = scaled * own_gain[None, span] + own_bias[None, span]
        ready.append(
            (jax.nn.silu(proj_g[:, span].astype(jnp.float32)) * scaled).astype(jnp.bfloat16)
        )
    retention_rows = jnp.concatenate(ready, axis=1) if heads > 1 else ready[0]
    retention_all = gather_line(retention_rows)

    def merge(ret_weight, conv_weight):
        return (
            jnp.dot(convolution_all, line_order(conv_weight), preferred_element_type=jnp.float32)
            + jnp.dot(retention_all, line_order(ret_weight), preferred_element_type=jnp.float32)
        ).astype(jnp.bfloat16)

    cols = retention_out_weight.shape[1]
    mixed = jnp.stack(
        [
            merge(retention_out_weight, convolution_out_weight),
            merge(ret_other, conv_other),
        ]
    )
    mixed = mixed.reshape(2, n_far, n_tp, fine, cols).transpose(2, 0, 1, 3, 4)
    mixed = lax.psum_scatter(
        mixed.reshape(2 * n_far * n_tp * fine, cols), "tp", scatter_dimension=0, tiled=True
    ).reshape(2, n_far, fine, cols)
    kept, arrived = mixed[0], across(mixed[1])
    home = jnp.where(
        side == 0, jnp.stack([kept, arrived]), jnp.stack([arrived, kept])
    ).reshape(n_sp, fine, cols)
    home = lax.all_to_all(home, "sp", 0, 0, tiled=True)
    return home.transpose(1, 0, 2).reshape(fine, n_sp * cols)


def with_halo(cells, sides, width):
    for axis, dim in sides:
        count = lax.axis_size(axis)
        ends = count - 1
        head = lax.slice_in_dim(cells, 0, width, axis=dim)
        tail = lax.slice_in_dim(cells, cells.shape[dim] - width, cells.shape[dim], axis=dim)
        cells = jnp.concatenate(
            [
                lax.ppermute(tail, axis, [(i, (i + 1) % count) for i in range(ends)]),
                cells,
                lax.ppermute(head, axis, [((i + 1) % count, i) for i in range(ends)]),
            ],
            axis=dim,
        )
    return cells


def rotate_at(rows, positions):
    half_dim = rows.shape[-1] // 2
    inverse = THETA ** (-jnp.arange(half_dim, dtype=jnp.float32) / half_dim)
    angles = positions.astype(jnp.float32)[:, None] * inverse[None, :]
    cosine = jnp.cos(angles)[:, None, :]
    sine = jnp.sin(angles)[:, None, :]
    widened = rows.astype(jnp.float32)
    first_half = widened[..., :half_dim]
    second_half = widened[..., half_dim:]
    turned = jnp.concatenate(
        [first_half * cosine - second_half * sine, second_half * cosine + first_half * sine],
        axis=-1,
    )
    return turned.astype(jnp.bfloat16)


def to_blocks(rows):
    return rows.reshape(rows.shape[0] // BLOCK, BLOCK, rows.shape[1], rows.shape[2]).transpose(
        2, 0, 1, 3
    )


def from_blocks(blocks):
    return blocks.transpose(1, 2, 0, 3).reshape(
        blocks.shape[1] * blocks.shape[2], blocks.shape[0], blocks.shape[3]
    )


def blockwise(queries, key_rows, values, log_decay, include_diag):
    block_len = queries.shape[2]
    position = jnp.arange(block_len, dtype=jnp.float32)
    distance = position[:, None] - position[None, :]
    allowed = distance >= 0 if include_diag else distance > 0
    inside = jnp.where(
        allowed[None], jnp.exp(log_decay[:, None, None] * jnp.maximum(distance, 0.0)[None]), 0.0
    )
    query_wide = queries.astype(jnp.float32)
    key_wide = key_rows.astype(jnp.float32)
    value_wide = values.astype(jnp.float32)
    scores = (
        jnp.einsum("hnqd,hnkd->hnqk", query_wide, key_wide, precision=lax.Precision.HIGHEST)
        * inside[:, None]
    )
    inner_part = jnp.einsum("hnqk,hnkd->hnqd", scores, value_wide, precision=lax.Precision.HIGHEST)
    toward_end = jnp.exp(log_decay[:, None] * (block_len - 1.0 - position)[None])
    block_states = jnp.einsum(
        "hnkd,hnke->hnde",
        key_wide * toward_end[:, None, :, None],
        value_wide,
        precision=lax.Precision.HIGHEST,
    )
    block_decay = jnp.exp(log_decay * block_len)[:, None, None]

    def advance(state_now, block_state):
        return (block_decay * state_now + block_state, state_now)

    initial = jnp.zeros(
        (block_states.shape[0], block_states.shape[2], block_states.shape[3]), jnp.float32
    )
    final_state, earlier = lax.scan(advance, initial, jnp.moveaxis(block_states, 1, 0))
    earlier = jnp.moveaxis(earlier, 0, 1)
    from_start = jnp.exp(log_decay[:, None] * (position + 1.0)[None])
    cross_part = jnp.einsum(
        "hnqd,hnde->hnqe",
        query_wide * from_start[:, None, :, None],
        earlier,
        precision=lax.Precision.HIGHEST,
    )
    return (inner_part + cross_part, final_state)


def group_norm(retained, group_gain, group_bias, gate_rows):
    row_mean = jnp.mean(retained, axis=-1, keepdims=True)
    centered = retained - row_mean
    variance = jnp.mean(centered * centered, axis=-1, keepdims=True)
    scaled = (centered * lax.rsqrt(variance + EPS)).reshape(retained.shape[0], -1)
    scaled = scaled * group_gain[None, :] + group_bias[None, :]
    return (jax.nn.silu(gate_rows.astype(jnp.float32)) * scaled).astype(jnp.bfloat16)


def shards_general(
    hidden_states,
    norm_gain,
    query_weight,
    key_weight,
    value_weight,
    output_gate_weight,
    unit_input_weight,
    unit_gate_weight,
    decay_forward,
    decay_backward,
    group_gain,
    group_bias,
    depth_kernel,
    depth_bias,
    channel_gain,
    channel_bias,
    retention_out_weight,
    convolution_out_weight,
):
    row_total = hidden_states.shape[0]
    whole = lax.all_gather(hidden_states, "tp", axis=1, tiled=True)
    widened = whole.astype(jnp.float32)
    normed = (
        widened
        * lax.rsqrt(jnp.mean(widened * widened, axis=-1, keepdims=True) + EPS)
        * norm_gain[None, :]
    ).astype(jnp.bfloat16)
    slabs = (
        lax.all_gather(query_weight, "sp", axis=0, tiled=True),
        lax.all_gather(key_weight, "sp", axis=0, tiled=True),
        lax.all_gather(value_weight, "sp", axis=0, tiled=True),
        lax.all_gather(output_gate_weight, "sp", axis=0, tiled=True),
        lax.all_gather(unit_input_weight, "sp", axis=0, tiled=True),
        lax.all_gather(unit_gate_weight, "sp", axis=0, tiled=True),
    )
    summed = tuple((jnp.dot(normed, slab, preferred_element_type=jnp.float32) for slab in slabs))
    proj_q, proj_k, proj_v, proj_g, proj_a, proj_b = tuple(
        (part_sum.astype(jnp.bfloat16) for part_sum in summed)
    )
    head_count = proj_q.shape[1] // HEAD_DIM
    device = lax.axis_index("sp")
    positions = device * row_total + jnp.arange(row_total, dtype=jnp.int32)
    queries = rotate_at(proj_q.reshape(row_total, head_count, HEAD_DIM), positions)
    key_rows = rotate_at(proj_k.reshape(row_total, head_count, HEAD_DIM), positions)
    values = proj_v.reshape(row_total, head_count, HEAD_DIM)
    log_forward = jax.nn.log_sigmoid(decay_forward)
    log_backward = jax.nn.log_sigmoid(decay_backward)
    ahead_local, state_ahead = blockwise(
        to_blocks(queries), to_blocks(key_rows), to_blocks(values), log_forward, True
    )
    behind_local, state_behind = blockwise(
        to_blocks(queries[::-1]),
        to_blocks(key_rows[::-1]),
        to_blocks(values[::-1]),
        log_backward,
        False,
    )
    slabs = (
        lax.all_gather(state_ahead[None].astype(jnp.bfloat16), "sp", axis=0, tiled=True).astype(
            jnp.float32
        ),
        lax.all_gather(state_behind[None].astype(jnp.bfloat16), "sp", axis=0, tiled=True).astype(
            jnp.float32
        ),
    )
    source = jnp.arange(slabs[0].shape[0], dtype=jnp.int32)
    gap_ahead = device - 1 - source
    gap_behind = source - device - 1
    weight_ahead = jnp.where(
        gap_ahead[:, None] >= 0,
        jnp.exp(
            log_forward[None, :]
            * row_total
            * jnp.maximum(gap_ahead, 0).astype(jnp.float32)[:, None]
        ),
        0.0,
    )
    weight_behind = jnp.where(
        gap_behind[:, None] >= 0,
        jnp.exp(
            log_backward[None, :]
            * row_total
            * jnp.maximum(gap_behind, 0).astype(jnp.float32)[:, None]
        ),
        0.0,
    )
    enter_ahead = jnp.zeros_like(state_ahead) + jnp.einsum(
        "jh,jhde->hde", weight_ahead, slabs[0], precision=lax.Precision.HIGHEST
    )
    enter_behind = jnp.zeros_like(state_behind) + jnp.einsum(
        "jh,jhde->hde", weight_behind, slabs[1], precision=lax.Precision.HIGHEST
    )
    local_position = jnp.arange(row_total, dtype=jnp.float32)
    lift_ahead = jnp.exp(log_forward[None, :] * (local_position + 1.0)[:, None])
    lift_behind = jnp.exp(log_backward[None, :] * (row_total - local_position)[:, None])
    query_wide = queries.astype(jnp.float32)
    carried = jnp.einsum(
        "shd,hde->she",
        query_wide * lift_ahead[:, :, None],
        enter_ahead,
        precision=lax.Precision.HIGHEST,
    )
    carried = carried + jnp.einsum(
        "shd,hde->she",
        query_wide * lift_behind[:, :, None],
        enter_behind,
        precision=lax.Precision.HIGHEST,
    )
    retained = from_blocks(ahead_local) + from_blocks(behind_local)[::-1] + carried
    retention_rows = group_norm(retained, group_gain, group_bias, proj_g)
    unit = (proj_a.astype(jnp.float32) * jax.nn.sigmoid(proj_b.astype(jnp.float32))).astype(
        jnp.bfloat16
    )
    half_kernel = (KERNEL - 1) // 2
    padded = with_halo(unit, (("sp", 0),), half_kernel)
    filtered = jnp.broadcast_to(depth_bias[None, :], (row_total, unit.shape[1]))
    for offset in range(KERNEL):
        filtered = filtered + depth_kernel[offset][None, :] * padded[
            offset : offset + row_total
        ].astype(jnp.float32)
    row_sum, row_squares = lax.psum(
        (jnp.sum(filtered, axis=1), jnp.sum(filtered * filtered, axis=1)), "tp"
    )
    row_mean = (row_sum / CONV_WIDTH)[:, None]
    variance = (row_squares / CONV_WIDTH)[:, None] - row_mean * row_mean
    leveled = (filtered - row_mean) * lax.rsqrt(variance + EPS) * channel_gain[
        None, :
    ] + channel_bias[None, :]
    convolution_rows = jax.nn.silu(leveled).astype(jnp.bfloat16)
    retention_full, convolution_full = (
        lax.all_gather(retention_out_weight, "sp", axis=1, tiled=True),
        lax.all_gather(convolution_out_weight, "sp", axis=1, tiled=True),
    )
    return lax.psum_scatter(
        (
            jnp.dot(retention_rows, retention_full, preferred_element_type=jnp.float32)
            + jnp.dot(convolution_rows, convolution_full, preferred_element_type=jnp.float32)
        ).astype(jnp.bfloat16),
        "tp",
        scatter_dimension=0,
        tiled=True,
    )


def solution(mesh):
    lines = mesh.shape["sp"] // SIDES
    head_groups = mesh.shape["tp"] * lines
    fits = mesh.shape["sp"] % SIDES == 0 and CONV_WIDTH % (head_groups * HEAD_DIM) == 0
    placed = (
        P("sp", "tp"),
        P(),
        P("sp", "tp"),
        P("sp", "tp"),
        P("sp", "tp"),
        P("sp", "tp"),
        P("sp", "tp"),
        P("sp", "tp"),
        P("tp"),
        P("tp"),
        P("tp"),
        P("tp"),
        P(None, "tp"),
        P("tp"),
        P("tp"),
        P("tp"),
        P("tp", "sp"),
        P("tp", "sp"),
    )
    return jax.shard_map(
        shards if fits else shards_general,
        mesh=mesh, in_specs=placed, out_specs=P(("sp", "tp"), None), check_vma=False
    )
```
